256 devices in a mesh: sp: 64 (over z, x, core), tp: 4 (over y).
Axes of the slice: x: 4, y: 4, z: 8, core: 2. Of those that a mesh axis runs over, the one named last changes fastest.
Arguments:
- tokens: bfloat16 [16384, 2048], P(('sp', 'tp')), may hold values from -6 to 6
- norm_gain: float32 [2048], replicated, may hold values from 0.1 to 1.9
- w_glu_a: bfloat16 [2048, 2048], P(None, 'tp'), may hold values from -0.125 to 0.125
- w_glu_b: bfloat16 [2048, 2048], P(None, 'tp'), may hold values from -0.125 to 0.125
- conv_taps: float32 [31, 2048], P(None, 'tp'), may hold values from -6 to 6
- ln_gain: float32 [2048], P('tp'), may hold values from 0.1 to 1.9
- w_query: bfloat16 [2048, 2048], P(None, 'tp'), may hold values from -0.125 to 0.125
- w_key: bfloat16 [2048, 512], P(None, 'tp'), may hold values from -0.125 to 0.125
- w_value: bfloat16 [2048, 512], P(None, 'tp'), may hold values from -0.125 to 0.125
- query_gain: float32 [16, 128], P('tp'), may hold values from 1 to 40
- key_gain: float32 [4, 128], P('tp'), may hold values from 0.1 to 1.9
- lam_head: float32 [16], P('tp'), may hold values from 0.3 to 0.8
- sub_gain: float32 [128], replicated, may hold values from 0.1 to 1.9
- w_out_conv: bfloat16 [2048, 2048], P('tp'), may hold values from -0.09375 to 0.09375
- w_out_attn: bfloat16 [2048, 2048], P('tp'), may hold values from -0.09375 to 0.09375
Outputs:
- mixed: bfloat16 [16384, 2048], P(('sp', 'tp'))
- log_sums: float32 [2, 16, 16384], P(None, 'tp', 'sp')
The draws below stay inside these ranges and needn't reach their ends.
All inputs are finite; a program needn't handle non-finite values.
Results may differ from the reference program's by a relative error of at most 0.015.
The reference program's roundings to bfloat16 on the way count: a program that leaves them out, or rounds other values in their place, can miss the bound.
Values may be sent and summed in bfloat16 or wider, within the bound.
No kernel may reach another device: no remote copies, remote signals or barrier semaphores. Data moves between devices by JAX's collectives and lax.ppermute only.
A program may use at most 128 MiB of HBM per device.

```python
import jax
import jax.numpy as jnp
from jax import lax

D = 2048
CONV_CH = 2048
KW = 31
HEADS = 16
KV_HEADS = 4
HEAD_DIM = 64
VALUE_DIM = 128
TOKENS = 16384
N_TP = 4


def draw_conv_taps(key, part):
    normal_part = jax.random.truncated_normal(key, -3.0, 3.0, (KW, CONV_CH), jnp.float32)
    channel_pos = jnp.arange(CONV_CH, dtype=jnp.float32) / CONV_CH
    growth = 3.0
    return normal_part * KW ** (-0.5) * jnp.exp(jnp.log(growth) * channel_pos)[None, :]


def draw_query_gain(key, part):
    gains = jax.random.uniform(key, (HEADS, 2 * HEAD_DIM), jnp.float32, 1.2, 1.9)
    return gains


def level_of(rng, extent, pieces, least, largest):
    def one(axis_at, blocks):
        draws = jax.random.uniform(jax.random.fold_in(jax.random.fold_in(rng, 6), axis_at), (blocks,), jnp.float32, least / len(pieces), largest / len(pieces))
        return jnp.repeat(jnp.exp(draws), extent[axis_at] // blocks).reshape((-1,) + (1,) * (len(extent) - axis_at - 1))

    loudness = one(*pieces[0])
    for cut in pieces[1:]:
        loudness = loudness * one(*cut)
    return loudness


def normal_values(key, shape, scale, reach, cuts=(), kind=jnp.bfloat16):
    factor_of = level_of(key, shape, cuts, -0.22, 0.18) if cuts else 1.0
    drawn = jax.random.normal(key, shape, jnp.float32) * scale * factor_of
    return jnp.minimum(jnp.maximum(drawn, -reach), reach).astype(kind)


def setup_inputs(seed: int = 0) -> dict:
    key_list = jax.random.split(jax.random.key(seed), 16)
    return {
        "tokens": normal_values(key_list[0], (TOKENS, D), 1.0, 6.0, ((0, 256),)),
        "norm_gain": jnp.clip(1.0 + 0.18 * jax.random.normal(key_list[1], (D,), jnp.float32), 0.1, 1.9),
        "w_glu_a": normal_values(key_list[2], (D, CONV_CH), D ** -0.5, 0.125, ((1, 4),)),
        "w_glu_b": normal_values(key_list[3], (D, CONV_CH), D ** -0.5, 0.125, ((1, 4),)),
        "conv_taps": draw_conv_taps(jax.random.fold_in(key_list[15], 71), 0),
        "ln_gain": jnp.clip(1.0 + 0.18 * jax.random.normal(key_list[5], (CONV_CH,), jnp.float32), 0.1, 1.9),
        "w_query": normal_values(key_list[6], (D, HEADS * 2 * HEAD_DIM), D ** -0.5, 0.125, ((1, 4),)),
        "w_key": normal_values(key_list[7], (D, KV_HEADS * 2 * HEAD_DIM), D ** -0.5, 0.125, ((1, 4),)),
        "w_value": normal_values(key_list[8], (D, KV_HEADS * VALUE_DIM), D ** -0.5, 0.125, ((1, 4),)),
        "query_gain": draw_query_gain(jax.random.fold_in(key_list[15], 71), 0),
        "key_gain": jnp.clip(1.0 + 0.18 * jax.random.normal(key_list[10], (KV_HEADS, 2 * HEAD_DIM), jnp.float32), 0.1, 1.9),
        "lam_head": jnp.clip(0.3 + 0.5 * jax.random.uniform(key_list[11], (HEADS,), jnp.float32) ** level_of(key_list[11], (HEADS,), ((0, 4),), -0.2, 0.2), 0.3, 0.8),
        "sub_gain": jnp.clip(1.0 + 0.18 * jax.random.normal(key_list[12], (VALUE_DIM,), jnp.float32), 0.1, 1.9),
        "w_out_conv": normal_values(key_list[13], (CONV_CH, D), (CONV_CH + HEADS * VALUE_DIM) ** -0.5, 0.09375, ((0, 4),)),
        "w_out_attn": normal_values(key_list[14], (HEADS * VALUE_DIM, D), (CONV_CH + HEADS * VALUE_DIM) ** -0.5, 0.09375, ((0, 4),)),
    }


def rms_scale(inputs_arr, gain_vec, epsilon):
    return inputs_arr * lax.rsqrt(lax.optimization_barrier(jnp.mean(inputs_arr * inputs_arr, axis=-1, keepdims=True)) + epsilon) * gain_vec

def reference(tokens, norm_gain, w_glu_a, w_glu_b, conv_taps, ln_gain, w_query, w_key, w_value, query_gain, key_gain, lam_head, sub_gain, w_out_conv, w_out_attn):
    seq_len = tokens.shape[0]
    normed = rms_scale(tokens.astype(jnp.float32), norm_gain, 1e-06).astype(jnp.bfloat16)
    glu_a = jnp.dot(normed, w_glu_a, preferred_element_type=jnp.float32)
    glu_b = jnp.dot(normed, w_glu_b, preferred_element_type=jnp.float32)
    gated_rows = (glu_a * jax.nn.sigmoid(glu_b)).astype(jnp.bfloat16)
    padded = jnp.concatenate([jnp.zeros((KW - 1, CONV_CH), jnp.bfloat16), gated_rows], axis=0)
    conv_sum = jnp.zeros((seq_len, CONV_CH), jnp.float32)
    for tap_idx in range(KW):
        conv_sum = conv_sum + conv_taps[tap_idx] * padded[tap_idx:tap_idx + seq_len].astype(jnp.float32)
    mean_val = lax.optimization_barrier(jnp.mean(conv_sum, axis=1, keepdims=True))
    mean_sq = lax.optimization_barrier(jnp.mean(conv_sum * conv_sum, axis=1, keepdims=True))
    normed_conv = (conv_sum - mean_val) * lax.rsqrt(mean_sq - mean_val * mean_val + 1e-05) * ln_gain
    conv_out = jax.nn.silu(normed_conv).astype(jnp.bfloat16)
    queries = jnp.dot(normed, w_query, preferred_element_type=jnp.float32).reshape(seq_len, HEADS, 2, HEAD_DIM)
    queries = rms_scale(queries, query_gain.reshape(HEADS, 2, HEAD_DIM), 1e-06).astype(jnp.bfloat16)
    key_heads = jnp.dot(normed, w_key, preferred_element_type=jnp.float32).reshape(seq_len, KV_HEADS, 2, HEAD_DIM)
    key_heads = rms_scale(key_heads, key_gain.reshape(KV_HEADS, 2, HEAD_DIM), 1e-06).astype(jnp.bfloat16)
    value_heads = jnp.dot(normed, w_value, preferred_element_type=jnp.float32).astype(jnp.bfloat16).reshape(seq_len, KV_HEADS, VALUE_DIM)
    group_size = HEADS // KV_HEADS
    query_rows = min(1024, seq_len)
    block_count = seq_len // query_rows
    key_pos = jnp.arange(seq_len, dtype=jnp.int32)

    def one_block(indices):
        head_idx, block_idx = indices
        kv_idx = head_idx // group_size
        row_first = block_idx * query_rows
        query_blk = lax.dynamic_slice(queries, (row_first, head_idx, jnp.int32(0), jnp.int32(0)), (query_rows, 1, 2, HEAD_DIM))[:, 0]
        key_head = lax.dynamic_index_in_dim(key_heads, kv_idx, 1, keepdims=False)
        value_head = lax.dynamic_index_in_dim(value_heads, kv_idx, 1, keepdims=False)
        query_pos = row_first + jnp.arange(query_rows, dtype=jnp.int32)
        visible = key_pos[None, :] <= query_pos[:, None]
        outputs = []
        log_list = []
        for map_idx in range(2):
            scores = jnp.dot(query_blk[:, map_idx], key_head[:, map_idx].T, preferred_element_type=jnp.float32) * HEAD_DIM ** (-0.5)
            scores = jnp.where(visible, scores, -jnp.inf)
            row_max = lax.optimization_barrier(jnp.max(scores, axis=1, keepdims=True))
            weights = jnp.exp(scores - row_max)
            row_total = lax.optimization_barrier(jnp.sum(weights, axis=1, keepdims=True))
            mixed_map = jnp.dot(weights.astype(jnp.bfloat16), value_head, preferred_element_type=jnp.float32) / row_total
            outputs.append(mixed_map)
            log_list.append((row_max + jnp.log(row_total))[:, 0])
        lam_value = lam_head[head_idx]
        diff_out = outputs[0] - lam_value * outputs[1]
        head_out = rms_scale(diff_out, sub_gain, 1e-06).astype(jnp.bfloat16)
        return (head_out, jnp.stack(log_list))
    head_ids = jnp.repeat(jnp.arange(HEADS, dtype=jnp.int32), block_count)
    block_ids = jnp.tile(jnp.arange(block_count, dtype=jnp.int32), HEADS)
    attn_blocks, lse_blocks = lax.map(one_block, (head_ids, block_ids))
    attn_out = attn_blocks.reshape(HEADS, block_count, query_rows, VALUE_DIM).transpose(1, 2, 0, 3).reshape(seq_len, HEADS * VALUE_DIM)
    log_sums = lse_blocks.reshape(HEADS, block_count, 2, query_rows).transpose(2, 0, 1, 3).reshape(2, HEADS, seq_len)
    conv_part = CONV_CH // N_TP
    attn_part = HEADS * VALUE_DIM // N_TP
    mixed_sum = jnp.zeros((seq_len, D), jnp.float32)
    for group_idx in range(N_TP):
        conv_lo = group_idx * conv_part
        attn_lo = group_idx * attn_part
        partial_value = jnp.dot(conv_out[:, conv_lo:conv_lo + conv_part], w_out_conv[conv_lo:conv_lo + conv_part], preferred_element_type=jnp.float32)
        partial_value = partial_value + jnp.dot(attn_out[:, attn_lo:attn_lo + attn_part], w_out_attn[attn_lo:attn_lo + attn_part], preferred_element_type=jnp.float32)
        mixed_sum = mixed_sum + lax.optimization_barrier(partial_value.astype(jnp.bfloat16)).astype(jnp.float32)
    return (mixed_sum.astype(jnp.bfloat16), log_sums)
```

```python
import functools

import jax
import jax.numpy as jnp
from jax import lax
from jax.experimental import pallas as pl
from jax.experimental.pallas import tpu as pltpu
from jax.sharding import PartitionSpec as P

KW = 31
NEG = -1e30
LOG2E = 1.4426950408889634
LN2 = 0.6931471805599453
UNROLL = 4


def sp_table(move):
    table = []
    for index in range(64):
        z, x, core = index // 8, (index // 2) % 4, index % 2
        nz, nx, nc = move(z, x, core)
        table.append((index, (nz % 8) * 8 + (nx % 4) * 2 + nc))
    return table


def sp_send(value, move):
    return lax.ppermute(value, "sp", sp_table(move))


def shifted(value, axis, steps):
    count = lax.axis_size(axis)
    leading, last = (max(0, -steps), min(count, count - steps))
    return lax.ppermute(value, axis, [(source, source + steps) for source in range(leading, last)])


def sent_to_all(value, axis):
    count = lax.axis_size(axis)
    return lax.all_to_all(
        jnp.broadcast_to(value[None], (count, *value.shape)), axis, 0, 0, tiled=True
    )


def rms_scale(inputs_arr, gain_vec, epsilon):
    return (
        inputs_arr
        * lax.rsqrt(jnp.mean(inputs_arr * inputs_arr, axis=-1, keepdims=True) + epsilon)
        * gain_vec
    )


def chunk_refs(pieces):
    return [(ref, row) for ref in pieces for row in range(0, ref.shape[0], 512)]


def slab_pass(chunks, q_ref, stats_ref, o_ref, s_refs, bias_ref):
    units = q_ref.shape[0]

    def score(unit, s_ref, at):
        ref, row = chunks[at]
        keys = ref[row : row + 256, :]
        s = jnp.dot(
            jnp.concatenate([keys, keys], axis=1), q_ref[unit], preferred_element_type=jnp.float32
        )
        if bias_ref is not None:
            s = s + bias_ref[unit // (units // 2), at * 256 : at * 256 + 256, :]
        s_ref[at * 256 : at * 256 + 256, :] = s
        return jnp.max(s.reshape(32, 8, 256), axis=0)

    def both(now, s_now, top, later, s_later):
        m_prev = stats_ref[now, 0:1, :]
        m_new = jnp.maximum(m_prev, jnp.max(top, axis=0, keepdims=True))
        alpha = jnp.exp2(m_prev - m_new)
        total, out, next_top = None, None, None
        for at, (ref, row) in enumerate(chunks):
            part = score(later, s_later, at)
            next_top = part if next_top is None else jnp.maximum(next_top, part)
            p = jnp.exp2(s_now[at * 256 : at * 256 + 256, :] - m_new)
            part = jnp.sum(p.reshape(32, 8, 256), axis=0)
            total = part if total is None else total + part
            vt = jnp.concatenate(
                [ref[row + 256 : row + 384, :], ref[row + 384 : row + 512, :]], axis=1
            )
            part = jnp.dot(vt, p.astype(jnp.bfloat16), preferred_element_type=jnp.float32)
            out = part if out is None else out + part
        stats_ref[now, 0:1, :] = m_new
        l_new = stats_ref[now, 1:2, :] * alpha + jnp.sum(total, axis=0, keepdims=True)
        stats_ref[now, 1:2, :] = l_new
        o_ref[now] = o_ref[now] * alpha + out
        return next_top

    top = None
    for at in range(len(chunks)):
        part = score(0, s_refs[0], at)
        top = part if top is None else jnp.maximum(top, part)

    def some(i, top):
        for j in range(UNROLL):
            unit = UNROLL * i + j
            later = jnp.minimum(unit + 1, units - 1)
            top = both(unit, s_refs[j % 2], top, later, s_refs[(j + 1) % 2])
        return top

    lax.fori_loop(0, units // UNROLL, some, top)


def spread_queries(q_in, q_ref):
    scale = LOG2E * q_in.shape[1] ** (-0.5)
    zero = jnp.zeros((64, 256), jnp.bfloat16)
    for unit in range(q_in.shape[0]):
        scaled = q_in[unit].astype(jnp.float32) * scale
        high = scaled.astype(jnp.bfloat16)
        low = (scaled - high.astype(jnp.float32)).astype(jnp.bfloat16)
        at = 64 * (unit % 2)
        for first, part in ((0, high), (128, low)):
            q_ref[unit, first + at : first + at + 64, :] = part
            q_ref[unit, first + 64 - at : first + 128 - at, :] = zero


def first_kernel(
    where_ref, q_in, own_ref, left_ref, right_ref, far_ref, stats_ref, o_ref, q_ref, s_a, s_b, bias_ref
):
    spread_queries(q_in, q_ref)
    x, core = where_ref[1], where_ref[2]
    units = q_ref.shape[0]
    stats_ref[...] = jnp.zeros_like(stats_ref)
    for unit in range(units):
        stats_ref[unit, 0:1, :] = jnp.full((1, 256), NEG, jnp.float32)
    o_ref[...] = jnp.zeros_like(o_ref)
    key_at = lax.broadcasted_iota(jnp.int32, (256, 256), 0)
    query_at = lax.broadcasted_iota(jnp.int32, (256, 256), 1)
    bias_ref[0, 0:256, :] = jnp.where(key_at <= query_at, 0.0, NEG)
    bias_ref[1, 0:256, :] = jnp.full((256, 256), jnp.where(core == 0, 0.0, NEG), jnp.float32)
    for at, step in ((1, 3), (2, 1), (3, 2)):
        seen = jnp.where(lax.rem(x + step, 4) < x, 0.0, NEG)
        for which in range(2):
            bias_ref[which, at * 256 : at * 256 + 256, :] = jnp.full((256, 256), seen, jnp.float32)
    chunks = chunk_refs((own_ref, left_ref, right_ref, far_ref))
    slab_pass(chunks, q_ref, stats_ref, o_ref, (s_a, s_b), bias_ref)


def slab_kernel(
    step, where_ref, q_in, a_ref, b_ref, stats_in, o_in, stats_ref, o_ref, q_ref, s_a, s_b
):
    z = where_ref[0]
    spread_queries(q_in, q_ref)

    def go(*pieces):
        slab_pass(chunk_refs(pieces), q_ref, stats_ref, o_ref, (s_a, s_b), None)

    if step == 4:
        pl.when(z >= 4)(lambda: go(a_ref, b_ref))
    else:
        pl.when(z >= step)(lambda: go(a_ref))
        pl.when(z + step >= 8)(lambda: go(b_ref))


def attend(where, q, pieces, state, step):
    units = q.shape[0]
    shapes = ((units, 8, 256), (units, 128, 256))
    vmem = pl.BlockSpec(memory_space=pltpu.VMEM)
    smem = pl.BlockSpec(memory_space=pltpu.SMEM)
    scratch = [pltpu.VMEM((units, 256, 256), jnp.bfloat16), pltpu.VMEM((1024, 256), jnp.float32), pltpu.VMEM((1024, 256), jnp.float32)]
    if step == 0:
        body, args, aliases = first_kernel, (where, q, *pieces), {}
        scratch.append(pltpu.VMEM((2, 1024, 256), jnp.float32))
        keys = 1024
    else:
        body, args = functools.partial(slab_kernel, step), (where, q, *pieces, *state)
        aliases = {4: 0, 5: 1}
        keys = sum(p.shape[0] for p in pieces) // 2
    return pl.pallas_call(
        body,
        out_shape=tuple(STATE(s) for s in shapes),
        in_specs=[smem] + [vmem] * (len(args) - 1),
        out_specs=(vmem, vmem),
        scratch_shapes=scratch,
        input_output_aliases=aliases,
        compiler_params=pltpu.CompilerParams(vmem_limit_bytes=24 << 20),
        cost_estimate=pl.CostEstimate(
            flops=2 * keys * 256 * units * 256, bytes_accessed=6 << 20, transcendentals=0
        ),
        name=f"attend_{step}",
    )(*args)


def STATE(shape):
    return pltpu.VMEM(shape, jnp.float32)


def on_device(
    tokens,
    norm_gain,
    w_glu_a,
    w_glu_b,
    conv_taps,
    ln_gain,
    w_query,
    w_key,
    w_value,
    query_gain,
    key_gain,
    lam_head,
    sub_gain,
    w_out_conv,
    w_out_attn,
):
    tp_count = lax.axis_size("tp")
    tok_dev = tokens.shape[0] * tp_count
    conv_local = w_glu_a.shape[1]
    heads = lam_head.shape[0]
    head_dim = key_gain.shape[1] // 2
    sp = lax.axis_index("sp")
    where = jnp.stack([sp // 8, (sp // 2) % 4, sp % 2]).astype(jnp.int32)

    normed = rms_scale(tokens.astype(jnp.float32), norm_gain, 1e-06).astype(jnp.bfloat16)
    rows_block = sent_to_all(normed, "tp").reshape(tok_dev, -1)

    key_part = jnp.dot(rows_block, w_key, preferred_element_type=jnp.float32).reshape(
        tok_dev, 2, head_dim
    )
    key_part = (
        rms_scale(key_part, key_gain.reshape(2, head_dim), 1e-06)
        .astype(jnp.bfloat16)
        .reshape(tok_dev, 2 * head_dim)
    )
    value_part = jnp.dot(rows_block, w_value, preferred_element_type=jnp.float32).astype(
        jnp.bfloat16
    )
    value_t = value_part.T
    own = jnp.concatenate([key_part, value_t[:, :128], value_t[:, 128:]], axis=0)

    left = sp_send(own, lambda z, x, c: (z, x + 1, c))
    right = sp_send(own, lambda z, x, c: (z, x - 1, c))
    far = sp_send(own, lambda z, x, c: (z, x + 2, c))
    slab = jnp.concatenate([own, left, right, far], axis=0)

    query_t = jnp.dot(rows_block, w_query, preferred_element_type=jnp.float32).T.reshape(
        heads * 2, head_dim, tok_dev
    )
    query_t = (
        query_t
        * lax.rsqrt(jnp.mean(query_t * query_t, axis=1, keepdims=True) + 1e-06)
        * query_gain.reshape(heads * 2, head_dim, 1)
    ).astype(jnp.bfloat16)
    partner_q = sp_send(query_t.reshape(heads * 128, tok_dev), lambda z, x, c: (z, x, 1 - c))
    both_q = jnp.concatenate([query_t, partner_q.reshape(query_t.shape)], axis=0)

    up = sp_send(slab, lambda z, x, c: (z + 1, x, c))
    down = sp_send(slab, lambda z, x, c: (z - 1, x, c))

    glu_a = jnp.dot(rows_block, w_glu_a, preferred_element_type=jnp.float32)
    glu_b = jnp.dot(rows_block, w_glu_b, preferred_element_type=jnp.float32)
    gated_rows = (glu_a * jax.nn.sigmoid(glu_b)).astype(jnp.bfloat16)
    prev_rows = shifted(gated_rows[tok_dev - (KW - 1) :], "sp", 1)
    padded = jnp.concatenate([prev_rows, gated_rows], axis=0)
    conv_sum = jnp.zeros((tok_dev, conv_local), jnp.float32)
    for tap_idx in range(KW):
        conv_sum = conv_sum + conv_taps[tap_idx] * padded[tap_idx : tap_idx + tok_dev].astype(
            jnp.float32
        )
    chan_total = conv_local * tp_count
    sums = jnp.concatenate([jnp.sum(conv_sum, axis=1), jnp.sum(conv_sum * conv_sum, axis=1)])
    sums = jnp.sum(sent_to_all(sums, "tp").reshape(tp_count, -1), axis=0)
    mean_val = (sums[:tok_dev] / chan_total)[:, None]
    mean_sq = (sums[tok_dev:] / chan_total)[:, None]
    conv_out = jax.nn.silu(
        (conv_sum - mean_val) * lax.rsqrt(mean_sq - mean_val * mean_val + 1e-05) * ln_gain
    ).astype(jnp.bfloat16)
    out_part = jnp.dot(conv_out, w_out_conv, preferred_element_type=jnp.float32)

    state = attend(where, both_q, (own, left, right, far), None, 0)
    for step in range(1, 5):
        if step < 4:
            new_up = sp_send(up if step < 3 else up[:1024], lambda z, x, c: (z + 1, x, c))
            new_down = sp_send(down if step < 3 else down[1024:], lambda z, x, c: (z - 1, x, c))
        state = attend(where, both_q, (up, down), state, step)
        if step < 4:
            up, down = new_up, new_down

    stats, acc = state
    half = 2 * heads
    swap = lambda z, x, c: (z, x, 1 - c)
    other_stats, other_acc = sp_send(stats[half:, :2], swap), sp_send(acc[half:], swap)
    m_a, l_a, m_b, l_b = stats[:half, 0], stats[:half, 1], other_stats[:, 0], other_stats[:, 1]
    m_all = jnp.maximum(m_a, m_b)
    w_a, w_b = jnp.exp2(m_a - m_all), jnp.exp2(m_b - m_all)
    l_all = l_a * w_a + l_b * w_b
    maps = (acc[:half] * w_a[:, None] + other_acc * w_b[:, None]) / l_all[:, None]
    maps = maps.reshape(heads, 2, 128, tok_dev)
    diff = maps[:, 0] - lam_head[:, None, None] * maps[:, 1]
    head_out = (
        diff
        * lax.rsqrt(jnp.mean(diff * diff, axis=1, keepdims=True) + 1e-06)
        * sub_gain[:, None]
    ).astype(jnp.bfloat16)
    attn_out = head_out.reshape(heads * 128, tok_dev).T
    log_sums = (m_all * LN2 + jnp.log(l_all)).reshape(heads, 2, tok_dev).transpose(1, 0, 2)

    out_part = out_part + jnp.dot(attn_out, w_out_attn, preferred_element_type=jnp.float32)
    out_part = lax.optimization_barrier(out_part.astype(jnp.bfloat16))
    blocks = lax.all_to_all(out_part.reshape(tp_count, -1, out_part.shape[1]), "tp", 0, 0, tiled=True)
    mixed = jnp.sum(blocks.astype(jnp.float32), axis=0).astype(jnp.bfloat16)
    return (mixed, log_sums)


def solution(mesh):
    return jax.shard_map(
        on_device,
        mesh=mesh,
        in_specs=(
            P(("sp", "tp"), None),
            P(),
            P(None, "tp"),
            P(None, "tp"),
            P(None, "tp"),
            P("tp"),
            P(None, "tp"),
            P(None, "tp"),
            P(None, "tp"),
            P("tp", None),
            P("tp", None),
            P("tp"),
            P(),
            P("tp", None),
            P("tp", None),
        ),
        out_specs=(P(("sp", "tp"), None), P(None, "tp", "sp")),
        check_vma=False,
    )
```

```python
import functools

import jax
import jax.numpy as jnp
from jax import lax
from jax.experimental import pallas as pl
from jax.experimental.pallas import tpu as pltpu
from jax.sharding import PartitionSpec as P

KW = 31
NEG = -1e30
LOG2E = 1.4426950408889634
LN2 = 0.6931471805599453
UNROLL = 2


def sp_table(move):
    table = []
    for index in range(64):
        z, x, core = index // 8, (index // 2) % 4, index % 2
        nz, nx, nc = move(z, x, core)
        table.append((index, (nz % 8) * 8 + (nx % 4) * 2 + nc))
    return table


def sp_send(value, move):
    return lax.ppermute(value, "sp", sp_table(move))


def mirrored(slabs):
    return [(z * 8 + r, (7 - z) * 8 + r) for z in slabs for r in range(8)]


def shifted(value, axis, steps):
    count = lax.axis_size(axis)
    leading, last = (max(0, -steps), min(count, count - steps))
    return lax.ppermute(value, axis, [(source, source + steps) for source in range(leading, last)])


def sent_to_all(value, axis):
    count = lax.axis_size(axis)
    return lax.all_to_all(
        jnp.broadcast_to(value[None], (count, *value.shape)), axis, 0, 0, tiled=True
    )


def chunk_refs(pieces):
    return [(ref, row) for ref in pieces for row in range(0, ref.shape[0], 512)]


def slab_pass(chunks, q_ref, state, s_refs, bias_ref, lo, hi):
    def score(pair, which, at):
        ref, row = chunks[at]
        keys = ref[row : row + 256, :]
        s = jnp.dot(
            jnp.concatenate([keys, keys], axis=1),
            q_ref[2 * pair + which],
            preferred_element_type=jnp.float32,
        )
        if bias_ref is not None:
            s = s + bias_ref[which, at * 256 : at * 256 + 256, :]
        s_refs[which][at * 256 : at * 256 + 256, :] = s
        return jnp.max(s.reshape(32, 8, 256), axis=0)

    def both(pair, which, top, later):
        stats_ref, o_ref = state[which], state[2 + which]
        m_prev = stats_ref[pair, 0:1, :]
        m_new = jnp.maximum(m_prev, jnp.max(top, axis=0, keepdims=True))
        alpha = jnp.exp2(m_prev - m_new)
        total, out, next_top = None, None, None
        for at, (ref, row) in enumerate(chunks):
            part = score(later, 1 - which, at)
            next_top = part if next_top is None else jnp.maximum(next_top, part)
            p = jnp.exp2(s_refs[which][at * 256 : at * 256 + 256, :] - m_new)
            part = jnp.sum(p.reshape(32, 8, 256), axis=0)
            total = part if total is None else total + part
            vt = jnp.concatenate(
                [ref[row + 256 : row + 384, :], ref[row + 384 : row + 512, :]], axis=1
            )
            part = jnp.dot(vt, p.astype(jnp.bfloat16), preferred_element_type=jnp.float32)
            out = part if out is None else out + part
        stats_ref[pair, 0:1, :] = m_new
        l_new = stats_ref[pair, 1:2, :] * alpha + jnp.sum(total, axis=0, keepdims=True)
        stats_ref[pair, 1:2, :] = l_new
        o_ref[pair] = o_ref[pair] * alpha + out
        return next_top

    top = None
    for at in range(len(chunks)):
        part = score(lo, 0, at)
        top = part if top is None else jnp.maximum(top, part)

    def some(i, top):
        pair = lo + i
        top = both(pair, 0, top, pair)
        return both(pair, 1, top, jnp.minimum(pair + 1, hi - 1))

    lax.fori_loop(0, hi - lo, some, top)


def spread_queries(q_in, q_ref):
    scale = LOG2E * q_in.shape[1] ** (-0.5)
    zero = jnp.zeros((64, 256), jnp.bfloat16)
    for unit in range(q_in.shape[0]):
        scaled = q_in[unit].astype(jnp.float32) * scale
        high = scaled.astype(jnp.bfloat16)
        low = (scaled - high.astype(jnp.float32)).astype(jnp.bfloat16)
        at = 64 * (unit // 2 % 2)
        for first, part in ((0, high), (128, low)):
            q_ref[unit, first + at : first + at + 64, :] = part
            q_ref[unit, first + 64 - at : first + 128 - at, :] = zero


def work_ends(z):
    moved = jnp.where((z == 0) | (z == 7), 2, jnp.where((z == 3) | (z == 4), 0, 1))
    own_end = jnp.where(z >= 4, 8 - 2 * moved, 8)
    guest_end = jnp.where(z < 4, 8 + 2 * moved, 8)
    return own_end, guest_end


def fill_bias(where_ref, bias_ref):
    x, core = where_ref[1], where_ref[2]
    key_at = lax.broadcasted_iota(jnp.int32, (256, 256), 0)
    query_at = lax.broadcasted_iota(jnp.int32, (256, 256), 1)
    bias_ref[0, 0:256, :] = jnp.where(key_at <= query_at, 0.0, NEG)
    bias_ref[1, 0:256, :] = jnp.full((256, 256), jnp.where(core == 0, 0.0, NEG), jnp.float32)
    for at, step in ((1, 3), (2, 1), (3, 2)):
        seen = jnp.where(lax.rem(x + step, 4) < x, 0.0, NEG)
        for which in range(2):
            bias_ref[which, at * 256 : at * 256 + 256, :] = jnp.full((256, 256), seen, jnp.float32)


def first_kernel(where_ref, q_in, own_ref, left_ref, right_ref, far_ref, *rest):
    state, (q_ref, s_a, s_b, bias_ref) = rest[:4], rest[4:]
    spread_queries(q_in, q_ref)
    for stats_ref, o_ref in zip(state[:2], state[2:]):
        stats_ref[...] = jnp.zeros_like(stats_ref)
        for pair in range(stats_ref.shape[0]):
            stats_ref[pair, 0:1, :] = jnp.full((1, 256), NEG, jnp.float32)
        o_ref[...] = jnp.zeros_like(o_ref)
    fill_bias(where_ref, bias_ref)
    own_end, guest_end = work_ends(where_ref[0])
    chunks = chunk_refs((own_ref, left_ref, right_ref, far_ref))
    slab_pass(chunks, q_ref, state, (s_a, s_b), bias_ref, 0, own_end)

    @pl.when(guest_end > 8)
    def _():
        slab_pass(chunks, q_ref, state, (s_a, s_b), None, 8, guest_end)


def slab_kernel(step, where_ref, q_in, a_ref, b_ref, *rest):
    state, (q_ref, s_a, s_b, bias_ref) = rest[4:8], rest[8:]
    for before, after in zip(rest[:4], state):
        after[...] = before[...]
    z = where_ref[0]
    spread_queries(q_in, q_ref)
    own_end, guest_end = work_ends(z)

    def go(slab, masked, *pieces):
        chunks = chunk_refs(pieces)
        own_seen, guest_seen = slab < z, (slab < 7 - z) & (z < 4)
        lo = jnp.where(own_seen, 0, 8)
        hi = jnp.where(guest_seen, guest_end, jnp.where(own_seen, own_end, 8))

        @pl.when(hi > lo)
        def _():
            slab_pass(chunks, q_ref, state, (s_a, s_b), None, lo, hi)

        if masked:

            @pl.when((slab == 7 - z) & (guest_end > 8))
            def _():
                fill_bias(where_ref, bias_ref)
                slab_pass(chunks, q_ref, state, (s_a, s_b), bias_ref, 8, guest_end)

    below, above = lax.rem(z + 8 - step, 8), lax.rem(z + step, 8)
    if step == 4:
        go(above, False, a_ref, b_ref)
    else:
        go(below, step in (1, 3), a_ref)
        go(above, step == 3, b_ref)


VMEM_SPEC = pl.BlockSpec(memory_space=pltpu.VMEM)
SMEM_SPEC = pl.BlockSpec(memory_space=pltpu.SMEM)


def plain_kernel(body, name, args, out_shape, scratch=(), aliases={}, flops=1 << 28, smem=1):
    return pl.pallas_call(
        body,
        out_shape=out_shape,
        in_specs=[SMEM_SPEC] * smem + [VMEM_SPEC] * (len(args) - smem),
        out_specs=jax.tree.map(lambda _: VMEM_SPEC, out_shape),
        scratch_shapes=scratch,
        input_output_aliases=aliases,
        compiler_params=pltpu.CompilerParams(vmem_limit_bytes=24 << 20),
        cost_estimate=pl.CostEstimate(flops=flops, bytes_accessed=2 << 20, transcendentals=0),
        name=name,
    )(*args)


def attend(where, q, pieces, state, step):
    units = q.shape[0]
    shapes = [(units // 2, 8, 256)] * 2 + [(units // 2, 128, 256)] * 2
    scratch = [
        pltpu.VMEM((units, 256, 256), jnp.bfloat16),
        pltpu.VMEM((1024, 256), jnp.float32),
        pltpu.VMEM((1024, 256), jnp.float32),
        pltpu.VMEM((2, 1024, 256), jnp.float32),
    ]
    if step == 0:
        body, args, aliases, keys = first_kernel, (where, q, *pieces), {}, 1024
    else:
        body, args = functools.partial(slab_kernel, step), (where, q, *pieces, *state)
        aliases = {4 + k: k for k in range(4)} if step < 4 else {}
        keys = sum(p.shape[0] for p in pieces) // 2
    kind = jax.ShapeDtypeStruct if step == 4 else pltpu.VMEM
    out_shape = tuple(kind(s, jnp.float32) for s in shapes)
    flops = keys * 256 * units * 256
    return plain_kernel(body, f"attend_{step}", args, out_shape, scratch, aliases, flops)


def front_kernel(where_ref, own_ref, left_ref, right_ref, far_ref, gain_ref, wk_ref, wv_ref, key_gain_ref, normed_ref, kv_ref):
    t = where_ref[3]
    for ref, step in ((own_ref, 0), (left_ref, 3), (right_ref, 1), (far_ref, 2)):
        row = pl.multiple_of(lax.rem(t + step, 4) * 64, 64)
        rows = ref[...].astype(jnp.float32)
        mean = jnp.mean(rows * rows, axis=1, keepdims=True)
        normed_ref[pl.ds(row, 64), :] = (rows * lax.rsqrt(mean + 1e-06) * gain_ref[...]).astype(
            jnp.bfloat16
        )
    normed = normed_ref[...]
    keys = jnp.dot(normed, wk_ref[...], preferred_element_type=jnp.float32)
    first = lax.broadcasted_iota(jnp.int32, keys.shape, 1) < 64
    square = keys * keys
    mean_a = jnp.sum(jnp.where(first, square, 0.0), axis=1, keepdims=True)
    mean_b = jnp.sum(jnp.where(first, 0.0, square), axis=1, keepdims=True)
    scale = jnp.where(
        first, lax.rsqrt(mean_a * (1 / 64) + 1e-06), lax.rsqrt(mean_b * (1 / 64) + 1e-06)
    )
    kv_ref[0:256, :] = (keys * scale * key_gain_ref[...]).astype(jnp.bfloat16)
    values = jnp.dot(normed, wv_ref[...], preferred_element_type=jnp.float32)
    for half in range(2):
        turned = values[half * 128 : half * 128 + 128, :].T
        kv_ref[256 + half * 128 : 384 + half * 128, :] = turned.astype(jnp.bfloat16)


def query_kernel(normed_ref, wq_ref, gain_ref, q_ref):
    normed = normed_ref[...]
    for part in range(wq_ref.shape[1] // 256):
        got = jnp.dot(
            normed, wq_ref[:, part * 256 : part * 256 + 256], preferred_element_type=jnp.float32
        )
        turned = got.T
        for k in range(4):
            at = part * 256 + k * 64
            q = turned[k * 64 : k * 64 + 64, :]
            mean = jnp.mean(q * q, axis=0, keepdims=True)
            q = q * lax.rsqrt(mean + 1e-06) * gain_ref[at : at + 64, :]
            q_ref[at : at + 64, :] = q.astype(jnp.bfloat16)


def finish_kernel(lam_ref, gain_ref, stats_a, acc_a, stats_b, acc_b, head_ref, log_ref):
    for head in range(head_ref.shape[0]):
        maps = []
        for half in range(2):
            pair = 2 * head + half
            m_a, m_b = stats_a[pair, 0:1, :], stats_b[pair, 0:1, :]
            m_all = jnp.maximum(m_a, m_b)
            w_a, w_b = jnp.exp2(m_a - m_all), jnp.exp2(m_b - m_all)
            l_all = stats_a[pair, 1:2, :] * w_a + stats_b[pair, 1:2, :] * w_b
            log_ref[pair, 0:1, :] = m_all * LN2 + jnp.log(l_all)
            maps.append((acc_a[pair] * w_a + acc_b[pair] * w_b) * (1.0 / l_all))
        diff = maps[0] - lam_ref[head] * maps[1]
        mean = jnp.mean(diff * diff, axis=0, keepdims=True)
        head_ref[head] = (diff * lax.rsqrt(mean + 1e-06) * gain_ref[...]).astype(jnp.bfloat16)


def on_device(
    tokens,
    norm_gain,
    w_glu_a,
    w_glu_b,
    conv_taps,
    ln_gain,
    w_query,
    w_key,
    w_value,
    query_gain,
    key_gain,
    lam_head,
    sub_gain,
    w_out_conv,
    w_out_attn,
):
    tp_count = lax.axis_size("tp")
    tok_dev = tokens.shape[0] * tp_count
    conv_local = w_glu_a.shape[1]
    heads = lam_head.shape[0]
    head_dim = key_gain.shape[1] // 2
    sp = lax.axis_index("sp")
    where = jnp.stack([sp // 8, (sp // 2) % 4, sp % 2, lax.axis_index("tp")]).astype(jnp.int32)

    rows_of = [
        lax.ppermute(tokens, "tp", [(t, (t + step) % 4) for t in range(4)]) for step in (2, 1, 3)
    ]
    normed_shape = jax.ShapeDtypeStruct((tok_dev, tokens.shape[1]), jnp.bfloat16)
    rows_block, own = plain_kernel(
        front_kernel,
        "front",
        (
            where,
            tokens,
            rows_of[1],
            rows_of[2],
            rows_of[0],
            norm_gain[None],
            w_key,
            w_value,
            key_gain,
        ),
        (normed_shape, jax.ShapeDtypeStruct((512, 128), jnp.bfloat16)),
    )

    query_t = plain_kernel(
        query_kernel,
        "queries",
        (rows_block, w_query, query_gain.reshape(-1, 1)),
        jax.ShapeDtypeStruct((w_query.shape[1], tok_dev), jnp.bfloat16),
        smem=0,
    )
    swap = lambda z, x, c: (z, x, 1 - c)
    query_t = query_t.reshape(heads, 2 * head_dim, tok_dev)
    given = jnp.stack([query_t[3], query_t[2]])
    guest = lax.ppermute(given, "sp", mirrored((7, 6, 5)))
    partner_q = sp_send(query_t, swap)
    left = sp_send(own, lambda z, x, c: (z, x + 1, c))
    right = sp_send(own, lambda z, x, c: (z, x - 1, c))
    far = sp_send(own, lambda z, x, c: (z, x + 2, c))
    guest_early, rows_block = lax.optimization_barrier((guest, rows_block))
    glu_a = jnp.dot(rows_block, w_glu_a, preferred_element_type=jnp.float32)
    glu_b = jnp.dot(rows_block, w_glu_b, preferred_element_type=jnp.float32)
    gated_rows = (glu_a * jax.nn.sigmoid(glu_b)).astype(jnp.bfloat16)
    prev_rows = shifted(gated_rows[tok_dev - (KW - 1) :], "sp", 1)
    partner_guest = sp_send(guest_early, swap)
    mine = jnp.concatenate([query_t, guest_early], axis=0).reshape(-1, head_dim, tok_dev)
    other = jnp.concatenate([partner_q, partner_guest], axis=0).reshape(-1, head_dim, tok_dev)
    both_q = jnp.stack([mine, other], axis=1).reshape(-1, head_dim, tok_dev)
    slab = jnp.concatenate([own, left, right, far], axis=0)

    slab, gated_rows = lax.optimization_barrier((slab, gated_rows))
    up = sp_send(slab, lambda z, x, c: (z + 1, x, c))
    down = sp_send(slab, lambda z, x, c: (z - 1, x, c))

    padded = jnp.concatenate([prev_rows, gated_rows], axis=0)
    conv_sum = jnp.zeros((tok_dev, conv_local), jnp.float32)
    for tap_idx in range(KW):
        conv_sum = conv_sum + conv_taps[tap_idx] * padded[tap_idx : tap_idx + tok_dev].astype(
            jnp.float32
        )
    chan_total = conv_local * tp_count
    sums = jnp.concatenate([jnp.sum(conv_sum, axis=1), jnp.sum(conv_sum * conv_sum, axis=1)])
    where_0, sums = lax.optimization_barrier((where, sums))
    sums = jnp.sum(sent_to_all(sums, "tp").reshape(tp_count, -1), axis=0)
    mean_val = (sums[:tok_dev] / chan_total)[:, None]
    mean_sq = (sums[tok_dev:] / chan_total)[:, None]
    conv_out = jax.nn.silu(
        (conv_sum - mean_val) * lax.rsqrt(mean_sq - mean_val * mean_val + 1e-05) * ln_gain
    ).astype(jnp.bfloat16)
    out_part = jnp.dot(conv_out, w_out_conv, preferred_element_type=jnp.float32)

    where_2, out_part = lax.optimization_barrier((where, out_part))

    state = attend(where_0, both_q, (own, left, right, far), None, 0)
    for step in range(1, 5):
        up, down, first = lax.optimization_barrier((up, down, state[0]))
        state = (first, *state[1:])
        if step < 4:
            new_up = sp_send(up if step < 3 else up[:1024], lambda z, x, c: (z + 1, x, c))
            new_down = sp_send(down if step < 3 else down[1024:], lambda z, x, c: (z - 1, x, c))
        state = attend(where if step == 1 else where_2, both_q, (up, down), state, step)
        if step < 4:
            up, down = new_up, new_down

    other_stats, other_acc = sp_send(state[1], swap), sp_send(state[3], swap)
    lam_all = jnp.concatenate([lam_head, lam_head[3:], lam_head[2:3]])
    pairs = state[0].shape[0]
    head_out, logs = plain_kernel(
        finish_kernel,
        "finish",
        (lam_all, sub_gain[:, None], state[0], state[2], other_stats, other_acc),
        (
            jax.ShapeDtypeStruct((pairs // 2, 128, tok_dev), jnp.bfloat16),
            jax.ShapeDtypeStruct((pairs, 8, tok_dev), jnp.float32),
        ),
    )
    logs = logs[:, 0].reshape(-1, 2, tok_dev)
    back_out = lax.ppermute(head_out[heads:], "sp", mirrored((0, 1, 2)))
    back_logs = lax.ppermute(logs[heads:], "sp", mirrored((0, 1, 2)))
    z = where[0]

    def with_guests(mine, back):
        third = jnp.where(z == 7, back[1], mine[2])
        fourth = jnp.where(z >= 5, back[0], mine[3])
        return jnp.concatenate([mine[:2], third[None], fourth[None]], axis=0)

    attn_t = with_guests(head_out, back_out).reshape(heads * 128, tok_dev)
    log_sums = with_guests(logs, back_logs).transpose(1, 0, 2)

    out_part = out_part + lax.dot_general(
        attn_t, w_out_attn, (((0,), (0,)), ((), ())), preferred_element_type=jnp.float32
    )
    out_part = lax.optimization_barrier(out_part.astype(jnp.bfloat16))
    blocks = lax.all_to_all(out_part.reshape(tp_count, -1, out_part.shape[1]), "tp", 0, 0, tiled=True)
    mixed = jnp.sum(blocks.astype(jnp.float32), axis=0).astype(jnp.bfloat16)
    return (mixed, log_sums)


def solution(mesh):
    return jax.shard_map(
        on_device,
        mesh=mesh,
        in_specs=(
            P(("sp", "tp"), None),
            P(),
            P(None, "tp"),
            P(None, "tp"),
            P(None, "tp"),
            P("tp"),
            P(None, "tp"),
            P(None, "tp"),
            P(None, "tp"),
            P("tp", None),
            P("tp", None),
            P("tp"),
            P(),
            P("tp", None),
            P("tp", None),
        ),
        out_specs=(P(("sp", "tp"), None), P(None, "tp", "sp")),
        check_vma=False,
    )
```

```python
import functools

import jax
import jax.numpy as jnp
from jax import lax
from jax.experimental import pallas as pl
from jax.experimental.pallas import tpu as pltpu
from jax.sharding import PartitionSpec as P

KW = 31
NEG = -1e30
LOG2E = 1.4426950408889634
LN2 = 0.6931471805599453
UNROLL = 2


def sp_table(move):
    table = []
    for index in range(64):
        z, x, core = index // 8, (index // 2) % 4, index % 2
        nz, nx, nc = move(z, x, core)
        table.append((index, (nz % 8) * 8 + (nx % 4) * 2 + nc))
    return table


def sp_send(value, move):
    return lax.ppermute(value, "sp", sp_table(move))


def mirrored(slabs):
    return [(z * 8 + r, (7 - z) * 8 + r) for z in slabs for r in range(8)]


def shifted(value, axis, steps):
    count = lax.axis_size(axis)
    leading, last = (max(0, -steps), min(count, count - steps))
    return lax.ppermute(value, axis, [(source, source + steps) for source in range(leading, last)])


def sent_to_all(value, axis):
    count = lax.axis_size(axis)
    return lax.all_to_all(
        jnp.broadcast_to(value[None], (count, *value.shape)), axis, 0, 0, tiled=True
    )


def chunk_refs(pieces):
    return [(ref, row) for ref in pieces for row in range(0, ref.shape[0], 512)]


def slab_pass(chunks, q_ref, state, s_refs, bias_ref, lo, hi, plane=None):
    def score(pair, which, at):
        ref, row = chunks[at]
        keys = ref[row : row + 256, :]
        s = jnp.dot(
            jnp.concatenate([keys, keys], axis=1),
            q_ref[2 * pair + which],
            preferred_element_type=jnp.float32,
        )
        if bias_ref is not None:
            s = s + bias_ref[plane(pair, which), at * 256 : at * 256 + 256, :]
        s_refs[which][at * 256 : at * 256 + 256, :] = s
        return jnp.max(s.reshape(32, 8, 256), axis=0)

    def both(pair, which, top, later):
        stats_ref, o_ref = state[which], state[2 + which]
        m_prev = stats_ref[pair, 0:1, :]
        m_new = jnp.maximum(m_prev, jnp.max(top, axis=0, keepdims=True))
        alpha = jnp.exp2(m_prev - m_new)
        total, out, next_top = None, None, None
        for at, (ref, row) in enumerate(chunks):
            part = score(later, 1 - which, at)
            next_top = part if next_top is None else jnp.maximum(next_top, part)
            p = jnp.exp2(s_refs[which][at * 256 : at * 256 + 256, :] - m_new)
            part = jnp.sum(p.reshape(32, 8, 256), axis=0)
            total = part if total is None else total + part
            vt = jnp.concatenate(
                [ref[row + 256 : row + 384, :], ref[row + 384 : row + 512, :]], axis=1
            )
            part = jnp.dot(vt, p.astype(jnp.bfloat16), preferred_element_type=jnp.float32)
            out = part if out is None else out + part
        stats_ref[pair, 0:1, :] = m_new
        l_new = stats_ref[pair, 1:2, :] * alpha + jnp.sum(total, axis=0, keepdims=True)
        stats_ref[pair, 1:2, :] = l_new
        o_ref[pair] = o_ref[pair] * alpha + out
        return next_top

    top = None
    for at in range(len(chunks)):
        part = score(lo, 0, at)
        top = part if top is None else jnp.maximum(top, part)

    def some(i, top):
        for j in range(2):
            pair = lo + 2 * i + j
            top = both(pair, 0, top, pair)
            top = both(pair, 1, top, jnp.minimum(pair + 1, hi - 1))
        return top

    lax.fori_loop(0, (hi - lo) // 2, some, top)


def spread_queries(q_in, q_ref):
    scale = LOG2E * q_in.shape[1] ** (-0.5)
    zero = jnp.zeros((64, 256), jnp.bfloat16)
    for unit in range(q_in.shape[0]):
        scaled = q_in[unit].astype(jnp.float32) * scale
        high = scaled.astype(jnp.bfloat16)
        low = (scaled - high.astype(jnp.float32)).astype(jnp.bfloat16)
        at = 64 * (unit // 2 % 2)
        for first, part in ((0, high), (128, low)):
            q_ref[unit, first + at : first + at + 64, :] = part
            q_ref[unit, first + 64 - at : first + 128 - at, :] = zero


def work_ends(z):
    moved = jnp.where((z == 0) | (z == 7), 2, jnp.where((z == 3) | (z == 4), 0, 1))
    own_end = jnp.where(z >= 4, 8 - 2 * moved, 8)
    guest_end = jnp.where(z < 4, 8 + 2 * moved, 8)
    return own_end, guest_end


def fill_bias(where_ref, bias_ref):
    x, core = where_ref[1], where_ref[2]
    bias_ref[2] = jnp.zeros((1024, 256), jnp.float32)
    key_at = lax.broadcasted_iota(jnp.int32, (256, 256), 0)
    query_at = lax.broadcasted_iota(jnp.int32, (256, 256), 1)
    bias_ref[0, 0:256, :] = jnp.where(key_at <= query_at, 0.0, NEG)
    bias_ref[1, 0:256, :] = jnp.full((256, 256), jnp.where(core == 0, 0.0, NEG), jnp.float32)
    for at, step in ((1, 3), (2, 1), (3, 2)):
        seen = jnp.where(lax.rem(x + step, 4) < x, 0.0, NEG)
        for which in range(2):
            bias_ref[which, at * 256 : at * 256 + 256, :] = jnp.full((256, 256), seen, jnp.float32)


def first_kernel(where_ref, q_in, own_ref, left_ref, right_ref, far_ref, *rest):
    state, (q_ref, s_a, s_b, bias_ref) = rest[:4], rest[4:8]
    spread_queries(q_in, q_ref)
    for stats_ref, o_ref in zip(state[:2], state[2:]):
        stats_ref[...] = jnp.zeros_like(stats_ref)
        for pair in range(stats_ref.shape[0]):
            stats_ref[pair, 0:1, :] = jnp.full((1, 256), NEG, jnp.float32)
        o_ref[...] = jnp.zeros_like(o_ref)
    fill_bias(where_ref, bias_ref)
    own_end, guest_end = work_ends(where_ref[0])
    chunks = chunk_refs((own_ref, left_ref, right_ref, far_ref))
    plane = lambda pair, which: jnp.where(pair < 8, which, 2)
    end = jnp.where(guest_end > 8, guest_end, own_end)
    slab_pass(chunks, q_ref, state, (s_a, s_b), bias_ref, 0, end, plane)


def slab_kernel(step, where_ref, q_ref, a_ref, b_ref, *rest):
    state, (s_a, s_b, bias_ref) = rest[4:8], rest[8:]
    for before, after in zip(rest[:4], state):
        after[...] = before[...]
    z = where_ref[0]
    own_end, guest_end = work_ends(z)
    if step in (1, 3):
        fill_bias(where_ref, bias_ref)

    def go(slab, masked, *pieces):
        chunks = chunk_refs(pieces)
        own_seen, guest_seen = slab < z, (slab < 7 - z) & (z < 4)
        lo = jnp.where(own_seen, 0, 8)
        hi = jnp.where(guest_seen, guest_end, jnp.where(own_seen, own_end, 8))
        same = (slab == 7 - z) & (guest_end > 8)
        if masked:
            hi = jnp.where(same, guest_end, hi)

        @pl.when(hi > lo)
        def _():
            plane = lambda pair, which: jnp.where(same, which, 2)
            bias = bias_ref if masked else None
            slab_pass(chunks, q_ref, state, (s_a, s_b), bias, lo, hi, plane)

    below, above = lax.rem(z + 8 - step, 8), lax.rem(z + step, 8)
    if step == 4:
        go(above, False, a_ref, b_ref)
    else:
        go(below, step in (1, 3), a_ref)
        go(above, step == 3, b_ref)


VMEM_SPEC = pl.BlockSpec(memory_space=pltpu.VMEM)
HBM_SPEC = pl.BlockSpec(memory_space=pltpu.HBM)
SMEM_SPEC = pl.BlockSpec(memory_space=pltpu.SMEM)


def plain_kernel(
    body, name, args, out_shape, scratch=(), aliases={}, flops=1 << 28, smem=1, spec=pl.BlockSpec(),
    vmem=24, hbm=0
):
    return pl.pallas_call(
        body,
        out_shape=out_shape,
        in_specs=[SMEM_SPEC] * smem + [HBM_SPEC] * hbm + [spec] * (len(args) - smem - hbm),
        out_specs=jax.tree.map(lambda _: spec, out_shape),
        scratch_shapes=scratch,
        input_output_aliases=aliases,
        compiler_params=pltpu.CompilerParams(vmem_limit_bytes=vmem << 20),
        cost_estimate=pl.CostEstimate(flops=flops, bytes_accessed=2 << 20, transcendentals=0),
        name=name,
    )(*args)


def attend(where, q, pieces, state, step):
    units = 24
    shapes = [(units // 2, 8, 256)] * 2 + [(units // 2, 128, 256)] * 2
    scratch = [
        pltpu.VMEM((1024, 256), jnp.float32),
        pltpu.VMEM((1024, 256), jnp.float32),
        pltpu.VMEM((3, 1024, 256), jnp.float32),
    ]
    if step == 0:
        body, args, aliases, keys = first_kernel, (where, q, *pieces), {}, 1024
    else:
        body, args = functools.partial(slab_kernel, step), (where, q, *pieces, *state)
        aliases = {4 + k: k for k in range(4)} if step < 4 else {}
        keys = sum(p.shape[0] for p in pieces) // 2
    kind = jax.ShapeDtypeStruct if step == 4 else pltpu.VMEM
    out_shape = tuple(kind(s, jnp.float32) for s in shapes)
    if step == 0:
        out_shape = (*out_shape, pltpu.VMEM((units, 256, 256), jnp.bfloat16))
    flops = keys * 256 * units * 256
    return plain_kernel(
        body, f"attend_{step}", args, out_shape, scratch, aliases, flops, spec=VMEM_SPEC
    )


def front_kernel(where_ref, *refs):
    (left_ref, right_ref, far_ref, normed_ref, kv_ref), held = refs[5:10], refs[10:15]
    own_ref, gain_ref, wk_ref, wv_ref, key_gain_ref = held
    copies = [pltpu.make_async_copy(refs[k], held[k], refs[15].at[k]) for k in range(5)]
    for k in (1, 0, 2, 3, 4):
        copies[k].start()
    t = where_ref[3]
    copies[1].wait()
    for ref, step in ((left_ref, 3), (right_ref, 1), (far_ref, 2), (own_ref, 0)):
        if step == 0:
            copies[0].wait()
        row = pl.multiple_of(lax.rem(t + step, 4) * 64, 64)
        rows = ref[...].astype(jnp.float32)
        mean = jnp.mean(rows * rows, axis=1, keepdims=True)
        normed_ref[pl.ds(row, 64), :] = (rows * lax.rsqrt(mean + 1e-06) * gain_ref[...]).astype(
            jnp.bfloat16
        )
    for k in (2, 3, 4):
        copies[k].wait()
    normed = normed_ref[...]
    keys = jnp.dot(normed, wk_ref[...], preferred_element_type=jnp.float32)
    first = lax.broadcasted_iota(jnp.int32, keys.shape, 1) < 64
    square = keys * keys
    mean_a = jnp.sum(jnp.where(first, square, 0.0), axis=1, keepdims=True)
    mean_b = jnp.sum(jnp.where(first, 0.0, square), axis=1, keepdims=True)
    scale = jnp.where(
        first, lax.rsqrt(mean_a * (1 / 64) + 1e-06), lax.rsqrt(mean_b * (1 / 64) + 1e-06)
    )
    kv_ref[0:256, :] = (keys * scale * key_gain_ref[...]).astype(jnp.bfloat16)
    values = jnp.dot(normed, wv_ref[...], preferred_element_type=jnp.float32)
    for half in range(2):
        turned = values[half * 128 : half * 128 + 128, :].T
        kv_ref[256 + half * 128 : 384 + half * 128, :] = turned.astype(jnp.bfloat16)


def query_kernel(normed_ref, wq_ref, gain_ref, q_ref):
    normed = normed_ref[...]
    for part in range(wq_ref.shape[1] // 256):
        got = jnp.dot(
            normed, wq_ref[:, part * 256 : part * 256 + 256], preferred_element_type=jnp.float32
        )
        turned = got.T
        for k in range(4):
            at = part * 256 + k * 64
            q = turned[k * 64 : k * 64 + 64, :]
            mean = jnp.mean(q * q, axis=0, keepdims=True)
            q = q * lax.rsqrt(mean + 1e-06) * gain_ref[at : at + 64, :]
            q_ref[at : at + 64, :] = q.astype(jnp.bfloat16)


def finish_kernel(lam_ref, gain_ref, stats_a, acc_a, stats_b, acc_b, head_ref, log_ref):
    for head in range(head_ref.shape[0]):
        maps = []
        for half in range(2):
            pair = 2 * head + half
            m_a, m_b = stats_a[pair, 0:1, :], stats_b[pair, 0:1, :]
            m_all = jnp.maximum(m_a, m_b)
            w_a, w_b = jnp.exp2(m_a - m_all), jnp.exp2(m_b - m_all)
            l_all = stats_a[pair, 1:2, :] * w_a + stats_b[pair, 1:2, :] * w_b
            log_ref[pair, 0:1, :] = m_all * LN2 + jnp.log(l_all)
            maps.append((acc_a[pair] * w_a + acc_b[pair] * w_b) * (1.0 / l_all))
        diff = maps[0] - lam_ref[(0, 1, 2, 3, 3, 2)[head]] * maps[1]
        mean = jnp.mean(diff * diff, axis=0, keepdims=True)
        head_ref[head] = (diff * lax.rsqrt(mean + 1e-06) * gain_ref[...]).astype(jnp.bfloat16)


def on_device(
    tokens,
    norm_gain,
    w_glu_a,
    w_glu_b,
    conv_taps,
    ln_gain,
    w_query,
    w_key,
    w_value,
    query_gain,
    key_gain,
    lam_head,
    sub_gain,
    w_out_conv,
    w_out_attn,
):
    tp_count = lax.axis_size("tp")
    tok_dev = tokens.shape[0] * tp_count
    conv_local = w_glu_a.shape[1]
    heads = lam_head.shape[0]
    head_dim = key_gain.shape[1] // 2
    sp = lax.axis_index("sp")
    where = jnp.stack([sp // 8, (sp // 2) % 4, sp % 2, lax.axis_index("tp")]).astype(jnp.int32)

    rows_of = [
        lax.ppermute(tokens, "tp", [(t, (t + step) % 4) for t in range(4)]) for step in (2, 1, 3)
    ]
    normed_shape = jax.ShapeDtypeStruct((tok_dev, tokens.shape[1]), jnp.bfloat16)
    rows_block, own = plain_kernel(
        front_kernel,
        "front",
        (
            where,
            tokens,
            norm_gain[None],
            w_key,
            w_value,
            key_gain,
            rows_of[1],
            rows_of[2],
            rows_of[0],
        ),
        (normed_shape, jax.ShapeDtypeStruct((512, 128), jnp.bfloat16)),
        scratch=[
            pltpu.VMEM(tokens.shape, jnp.bfloat16),
            pltpu.VMEM((1, tokens.shape[1]), jnp.float32),
            pltpu.VMEM(w_key.shape, jnp.bfloat16),
            pltpu.VMEM(w_value.shape, jnp.bfloat16),
            pltpu.VMEM(key_gain.shape, jnp.float32),
            pltpu.SemaphoreType.DMA((5,)),
        ],
        hbm=5,
    )

    query_t = plain_kernel(
        query_kernel,
        "queries",
        (rows_block, w_query, query_gain.reshape(-1, 1)),
        jax.ShapeDtypeStruct((w_query.shape[1], tok_dev), jnp.bfloat16),
        smem=0,
    )
    swap = lambda z, x, c: (z, x, 1 - c)
    query_t = query_t.reshape(heads, 2 * head_dim, tok_dev)
    given = jnp.stack([query_t[3], query_t[2]])
    guest = lax.ppermute(given, "sp", mirrored((7, 6, 5)))
    partner_q = sp_send(query_t, swap)
    left = sp_send(own, lambda z, x, c: (z, x + 1, c))
    right = sp_send(own, lambda z, x, c: (z, x - 1, c))
    far = sp_send(own, lambda z, x, c: (z, x + 2, c))
    guest_early, rows_block = lax.optimization_barrier((guest, rows_block))
    glu_a = jnp.dot(rows_block, w_glu_a, preferred_element_type=jnp.float32)
    glu_b = jnp.dot(rows_block, w_glu_b, preferred_element_type=jnp.float32)
    gated_rows = (glu_a * jax.nn.sigmoid(glu_b)).astype(jnp.bfloat16)
    prev_rows = shifted(gated_rows[tok_dev - (KW - 1) :], "sp", 1)
    partner_guest = sp_send(guest_early, swap)
    mine = jnp.concatenate([query_t, guest_early], axis=0).reshape(-1, head_dim, tok_dev)
    other = jnp.concatenate([partner_q, partner_guest], axis=0).reshape(-1, head_dim, tok_dev)
    both_q = jnp.stack([mine, other], axis=1).reshape(-1, head_dim, tok_dev)
    slab = jnp.concatenate([own, left, right, far], axis=0)

    slab, gated_rows = lax.optimization_barrier((slab, gated_rows))
    up = sp_send(slab, lambda z, x, c: (z + 1, x, c))
    down = sp_send(slab, lambda z, x, c: (z - 1, x, c))

    padded = jnp.concatenate([prev_rows, gated_rows], axis=0)
    conv_sum = jnp.zeros((tok_dev, conv_local), jnp.float32)
    for tap_idx in range(KW):
        conv_sum = conv_sum + conv_taps[tap_idx] * padded[tap_idx : tap_idx + tok_dev].astype(
            jnp.float32
        )
    chan_total = conv_local * tp_count
    sums = jnp.concatenate([jnp.sum(conv_sum, axis=1), jnp.sum(conv_sum * conv_sum, axis=1)])
    where_0, sums = lax.optimization_barrier((where, sums))
    sums = jnp.sum(sent_to_all(sums, "tp").reshape(tp_count, -1), axis=0)
    mean_val = (sums[:tok_dev] / chan_total)[:, None]
    mean_sq = (sums[tok_dev:] / chan_total)[:, None]
    conv_out = jax.nn.silu(
        (conv_sum - mean_val) * lax.rsqrt(mean_sq - mean_val * mean_val + 1e-05) * ln_gain
    ).astype(jnp.bfloat16)
    out_part = jnp.dot(conv_out, w_out_conv, preferred_element_type=jnp.float32)

    where_2, out_part = lax.optimization_barrier((where, out_part))

    *state, spread_q = attend(where, both_q, (own, left, right, far), None, 0)
    for step in range(1, 5):
        held = sums if step == 1 else behind
        up, down, held = lax.optimization_barrier((up, down, held))
        if step > 1:
            state = (held, *state[1:])
        if step < 4:
            new_up = sp_send(up if step < 3 else up[:1024], lambda z, x, c: (z + 1, x, c))
            new_down = sp_send(down if step < 3 else down[1024:], lambda z, x, c: (z - 1, x, c))
        behind = state[0]
        if step > 1:
            state = attend(where_2 if step == 3 else where, spread_q, pending, state, step - 1)
            behind = state[0]
        pending = (up, down)
        if step < 4:
            up, down = new_up, new_down
    state = attend(where_2, spread_q, pending, state, 4)

    other_stats, other_acc = sp_send(state[1], swap), sp_send(state[3], swap)
    pairs = state[0].shape[0]
    head_out, logs = plain_kernel(
        finish_kernel,
        "finish",
        (lam_head, sub_gain[:, None], state[0], state[2], other_stats, other_acc),
        (
            jax.ShapeDtypeStruct((pairs // 2, 128, tok_dev), jnp.bfloat16),
            jax.ShapeDtypeStruct((pairs, 8, tok_dev), jnp.float32),
        ),
    )
    logs = logs[:, 0].reshape(-1, 2, tok_dev)
    back_out = lax.ppermute(head_out[heads:], "sp", mirrored((0, 1, 2)))
    back_logs = lax.ppermute(logs[heads:], "sp", mirrored((0, 1, 2)))
    z = where[0]

    def with_guests(mine, back):
        third = jnp.where(z == 7, back[1], mine[2])
        fourth = jnp.where(z >= 5, back[0], mine[3])
        return jnp.concatenate([mine[:2], third[None], fourth[None]], axis=0)

    attn_t = with_guests(head_out, back_out).reshape(heads * 128, tok_dev)
    log_sums = with_guests(logs, back_logs).transpose(1, 0, 2)

    out_part = out_part + lax.dot_general(
        attn_t, w_out_attn, (((0,), (0,)), ((), ())), preferred_element_type=jnp.float32
    )
    out_part = lax.optimization_barrier(out_part.astype(jnp.bfloat16))
    blocks = lax.all_to_all(out_part.reshape(tp_count, -1, out_part.shape[1]), "tp", 0, 0, tiled=True)
    mixed = jnp.sum(blocks.astype(jnp.float32), axis=0).astype(jnp.bfloat16)
    return (mixed, log_sums)


def solution(mesh):
    return jax.shard_map(
        on_device,
        mesh=mesh,
        in_specs=(
            P(("sp", "tp"), None),
            P(),
            P(None, "tp"),
            P(None, "tp"),
            P(None, "tp"),
            P("tp"),
            P(None, "tp"),
            P(None, "tp"),
            P(None, "tp"),
            P("tp", None),
            P("tp", None),
            P("tp"),
            P(),
            P("tp", None),
            P("tp", None),
        ),
        out_specs=(P(("sp", "tp"), None), P(None, "tp", "sp")),
        check_vma=False,
    )
```

```python
import functools

import jax
import jax.numpy as jnp
from jax import lax
from jax.experimental import pallas as pl
from jax.experimental.pallas import tpu as pltpu
from jax.sharding import PartitionSpec as P

KW = 31
NEG = -1e30
LOG2E = 1.4426950408889634
LN2 = 0.6931471805599453
UNROLL = 2


def sp_table(move):
    table = []
    for index in range(64):
        z, x, core = index // 8, (index // 2) % 4, index % 2
        nz, nx, nc = move(z, x, core)
        table.append((index, (nz % 8) * 8 + (nx % 4) * 2 + nc))
    return table


def sp_send(value, move):
    return lax.ppermute(value, "sp", sp_table(move))


def mirrored(slabs):
    return [(z * 8 + r, (7 - z) * 8 + r) for z in slabs for r in range(8)]


def shifted(value, axis, steps):
    count = lax.axis_size(axis)
    leading, last = (max(0, -steps), min(count, count - steps))
    return lax.ppermute(value, axis, [(source, source + steps) for source in range(leading, last)])


def sent_to_all(value, axis):
    count = lax.axis_size(axis)
    return lax.all_to_all(
        jnp.broadcast_to(value[None], (count, *value.shape)), axis, 0, 0, tiled=True
    )


def chunk_refs(pieces):
    return [(ref, row) for ref in pieces for row in range(0, ref.shape[0], 512)]


def slab_pass(chunks, q_ref, state, s_refs, bias_ref, lo, hi, plane=None):
    def score(pair, which, at):
        ref, row = chunks[at]
        keys = ref[row : row + 256, :]
        s = jnp.dot(
            jnp.concatenate([keys, keys], axis=1),
            q_ref[2 * pair + which],
            preferred_element_type=jnp.float32,
        )
        if bias_ref is not None:
            s = s + bias_ref[plane(pair, which), at * 256 : at * 256 + 256, :]
        s_refs[which][at * 256 : at * 256 + 256, :] = s
        return jnp.max(s.reshape(32, 8, 256), axis=0)

    def both(pair, which, top, later):
        stats_ref, o_ref = state[which], state[2 + which]
        m_prev = stats_ref[pair, 0:1, :]
        m_new = jnp.maximum(m_prev, jnp.max(top, axis=0, keepdims=True))
        alpha = jnp.exp2(m_prev - m_new)
        total, out, next_top = None, None, None
        for at, (ref, row) in enumerate(chunks):
            part = score(later, 1 - which, at)
            next_top = part if next_top is None else jnp.maximum(next_top, part)
            p = jnp.exp2(s_refs[which][at * 256 : at * 256 + 256, :] - m_new)
            part = jnp.sum(p.reshape(32, 8, 256), axis=0)
            total = part if total is None else total + part
            vt = jnp.concatenate(
                [ref[row + 256 : row + 384, :], ref[row + 384 : row + 512, :]], axis=1
            )
            part = jnp.dot(vt, p.astype(jnp.bfloat16), preferred_element_type=jnp.float32)
            out = part if out is None else out + part
        stats_ref[pair, 0:1, :] = m_new
        l_new = stats_ref[pair, 1:2, :] * alpha + jnp.sum(total, axis=0, keepdims=True)
        stats_ref[pair, 1:2, :] = l_new
        o_ref[pair] = o_ref[pair] * alpha + out
        return next_top

    top = None
    for at in range(len(chunks)):
        part = score(lo, 0, at)
        top = part if top is None else jnp.maximum(top, part)

    def some(i, top):
        for j in range(2):
            pair = lo + 2 * i + j
            top = both(pair, 0, top, pair)
            top = both(pair, 1, top, jnp.minimum(pair + 1, hi - 1))
        return top

    lax.fori_loop(0, (hi - lo) // 2, some, top)


def spread_queries(q_in, q_ref):
    scale = LOG2E * q_in.shape[1] ** (-0.5)
    zero = jnp.zeros((64, 256), jnp.bfloat16)
    for unit in range(q_in.shape[0]):
        scaled = q_in[unit].astype(jnp.float32) * scale
        high = scaled.astype(jnp.bfloat16)
        low = (scaled - high.astype(jnp.float32)).astype(jnp.bfloat16)
        at = 64 * (unit // 2 % 2)
        for first, part in ((0, high), (128, low)):
            q_ref[unit, first + at : first + at + 64, :] = part
            q_ref[unit, first + 64 - at : first + 128 - at, :] = zero


def work_ends(z):
    moved = jnp.where((z == 0) | (z == 7), 2, jnp.where((z == 3) | (z == 4), 0, 1))
    own_end = jnp.where(z >= 4, 8 - 2 * moved, 8)
    guest_end = jnp.where(z < 4, 8 + 2 * moved, 8)
    return own_end, guest_end


def fill_bias(where_ref, bias_ref):
    x, core = where_ref[1], where_ref[2]
    bias_ref[2] = jnp.zeros((1024, 256), jnp.float32)
    key_at = lax.broadcasted_iota(jnp.int32, (256, 256), 0)
    query_at = lax.broadcasted_iota(jnp.int32, (256, 256), 1)
    bias_ref[0, 0:256, :] = jnp.where(key_at <= query_at, 0.0, NEG)
    bias_ref[1, 0:256, :] = jnp.full((256, 256), jnp.where(core == 0, 0.0, NEG), jnp.float32)
    for at, step in ((1, 3), (2, 1), (3, 2)):
        seen = jnp.where(lax.rem(x + step, 4) < x, 0.0, NEG)
        for which in range(2):
            bias_ref[which, at * 256 : at * 256 + 256, :] = jnp.full((256, 256), seen, jnp.float32)


def first_kernel(where_ref, q_in, own_ref, left_ref, right_ref, far_ref, *rest):
    state, (q_ref, s_a, s_b, bias_ref) = rest[:4], rest[4:8]
    spread_queries(q_in, q_ref)
    for stats_ref, o_ref in zip(state[:2], state[2:]):
        stats_ref[...] = jnp.zeros_like(stats_ref)
        for pair in range(stats_ref.shape[0]):
            stats_ref[pair, 0:1, :] = jnp.full((1, 256), NEG, jnp.float32)
        o_ref[...] = jnp.zeros_like(o_ref)
    fill_bias(where_ref, bias_ref)
    own_end, guest_end = work_ends(where_ref[0])
    chunks = chunk_refs((own_ref, left_ref, right_ref, far_ref))
    plane = lambda pair, which: jnp.where(pair < 8, which, 2)
    end = jnp.where(guest_end > 8, guest_end, own_end)
    slab_pass(chunks, q_ref, state, (s_a, s_b), bias_ref, 0, end, plane)


def slab_kernel(step, where_ref, q_ref, a_ref, b_ref, *rest):
    state, (s_a, s_b, bias_ref) = rest[4:8], rest[8:]
    for before, after in zip(rest[:4], state):
        after[...] = before[...]
    z = where_ref[0]
    own_end, guest_end = work_ends(z)
    if step in (1, 3):
        fill_bias(where_ref, bias_ref)

    def go(slab, masked, *pieces):
        chunks = chunk_refs(pieces)
        own_seen, guest_seen = slab < z, (slab < 7 - z) & (z < 4)
        lo = jnp.where(own_seen, 0, 8)
        hi = jnp.where(guest_seen, guest_end, jnp.where(own_seen, own_end, 8))
        same = (slab == 7 - z) & (guest_end > 8)
        if masked:
            hi = jnp.where(same, guest_end, hi)

        @pl.when(hi > lo)
        def _():
            plane = lambda pair, which: jnp.where(same, which, 2)
            bias = bias_ref if masked else None
            slab_pass(chunks, q_ref, state, (s_a, s_b), bias, lo, hi, plane)

    below, above = lax.rem(z + 8 - step, 8), lax.rem(z + step, 8)
    if step == 4:
        go(above, False, a_ref, b_ref)
    else:
        go(below, step in (1, 3), a_ref)
        go(above, step == 3, b_ref)


VMEM_SPEC = pl.BlockSpec(memory_space=pltpu.VMEM)
HBM_SPEC = pl.BlockSpec(memory_space=pltpu.HBM)
SMEM_SPEC = pl.BlockSpec(memory_space=pltpu.SMEM)


def plain_kernel(
    body, name, args, out_shape, scratch=(), aliases={}, flops=1 << 28, smem=1, spec=pl.BlockSpec(),
    vmem=24, hbm=0
):
    return pl.pallas_call(
        body,
        out_shape=out_shape,
        in_specs=[SMEM_SPEC] * smem + [HBM_SPEC] * hbm + [spec] * (len(args) - smem - hbm),
        out_specs=jax.tree.map(lambda _: spec, out_shape),
        scratch_shapes=scratch,
        input_output_aliases=aliases,
        compiler_params=pltpu.CompilerParams(vmem_limit_bytes=vmem << 20),
        cost_estimate=pl.CostEstimate(flops=flops, bytes_accessed=2 << 20, transcendentals=0),
        name=name,
    )(*args)


def attend(where, q, pieces, state, step):
    units = 24
    shapes = [(units // 2, 8, 256)] * 2 + [(units // 2, 128, 256)] * 2
    scratch = [
        pltpu.VMEM((1024, 256), jnp.float32),
        pltpu.VMEM((1024, 256), jnp.float32),
        pltpu.VMEM((3, 1024, 256), jnp.float32),
    ]
    if step == 0:
        body, args, aliases, keys = first_kernel, (where, q, *pieces), {}, 1024
    else:
        body, args = functools.partial(slab_kernel, step), (where, q, *pieces, *state)
        aliases = {4 + k: k for k in range(4)} if step < 4 else {}
        keys = sum(p.shape[0] for p in pieces) // 2
    kind = jax.ShapeDtypeStruct if step == 4 else pltpu.VMEM
    out_shape = tuple(kind(s, jnp.float32) for s in shapes)
    if step == 0:
        out_shape = (*out_shape, pltpu.VMEM((units, 256, 256), jnp.bfloat16))
    flops = keys * 256 * units * 256
    return plain_kernel(
        body, f"attend_{step}", args, out_shape, scratch, aliases, flops, spec=VMEM_SPEC
    )


def stage_kernel(*refs):
    for before, after in zip(refs[:5], refs[5:]):
        after[...] = before[...]


def front_kernel(
    where_ref, own_ref, gain_ref, wk_ref, wv_ref, key_gain_ref, left_ref, right_ref, far_ref,
    normed_ref, kv_ref
):
    t = where_ref[3]
    for ref, step in ((left_ref, 3), (right_ref, 1), (far_ref, 2), (own_ref, 0)):
        row = pl.multiple_of(lax.rem(t + step, 4) * 64, 64)
        rows = ref[...].astype(jnp.float32)
        mean = jnp.mean(rows * rows, axis=1, keepdims=True)
        normed_ref[pl.ds(row, 64), :] = (rows * lax.rsqrt(mean + 1e-06) * gain_ref[...]).astype(
            jnp.bfloat16
        )
    normed = normed_ref[...]
    keys = jnp.dot(normed, wk_ref[...], preferred_element_type=jnp.float32)
    first = lax.broadcasted_iota(jnp.int32, keys.shape, 1) < 64
    square = keys * keys
    mean_a = jnp.sum(jnp.where(first, square, 0.0), axis=1, keepdims=True)
    mean_b = jnp.sum(jnp.where(first, 0.0, square), axis=1, keepdims=True)
    scale = jnp.where(
        first, lax.rsqrt(mean_a * (1 / 64) + 1e-06), lax.rsqrt(mean_b * (1 / 64) + 1e-06)
    )
    kv_ref[0:256, :] = (keys * scale * key_gain_ref[...]).astype(jnp.bfloat16)
    values = jnp.dot(normed, wv_ref[...], preferred_element_type=jnp.float32)
    for half in range(2):
        turned = values[half * 128 : half * 128 + 128, :].T
        kv_ref[256 + half * 128 : 384 + half * 128, :] = turned.astype(jnp.bfloat16)


def query_kernel(normed_ref, wq_ref, gain_ref, q_ref):
    normed = normed_ref[...]
    for part in range(wq_ref.shape[1] // 256):
        got = jnp.dot(
            normed, wq_ref[:, part * 256 : part * 256 + 256], preferred_element_type=jnp.float32
        )
        turned = got.T
        for k in range(4):
            at = part * 256 + k * 64
            q = turned[k * 64 : k * 64 + 64, :]
            mean = jnp.mean(q * q, axis=0, keepdims=True)
            q = q * lax.rsqrt(mean + 1e-06) * gain_ref[at : at + 64, :]
            q_ref[at : at + 64, :] = q.astype(jnp.bfloat16)


def finish_kernel(lam_ref, gain_ref, stats_a, acc_a, stats_b, acc_b, head_ref, log_ref):
    for head in range(head_ref.shape[0]):
        maps = []
        for half in range(2):
            pair = 2 * head + half
            m_a, m_b = stats_a[pair, 0:1, :], stats_b[pair, 0:1, :]
            m_all = jnp.maximum(m_a, m_b)
            w_a, w_b = jnp.exp2(m_a - m_all), jnp.exp2(m_b - m_all)
            l_all = stats_a[pair, 1:2, :] * w_a + stats_b[pair, 1:2, :] * w_b
            log_ref[pair, 0:1, :] = m_all * LN2 + jnp.log(l_all)
            maps.append((acc_a[pair] * w_a + acc_b[pair] * w_b) * (1.0 / l_all))
        diff = maps[0] - lam_ref[(0, 1, 2, 3, 3, 2)[head]] * maps[1]
        mean = jnp.mean(diff * diff, axis=0, keepdims=True)
        head_ref[head] = (diff * lax.rsqrt(mean + 1e-06) * gain_ref[...]).astype(jnp.bfloat16)


def on_device(
    tokens,
    norm_gain,
    w_glu_a,
    w_glu_b,
    conv_taps,
    ln_gain,
    w_query,
    w_key,
    w_value,
    query_gain,
    key_gain,
    lam_head,
    sub_gain,
    w_out_conv,
    w_out_attn,
):
    tp_count = lax.axis_size("tp")
    tok_dev = tokens.shape[0] * tp_count
    conv_local = w_glu_a.shape[1]
    heads = lam_head.shape[0]
    head_dim = key_gain.shape[1] // 2
    sp = lax.axis_index("sp")
    where = jnp.stack([sp // 8, (sp // 2) % 4, sp % 2, lax.axis_index("tp")]).astype(jnp.int32)

    rows_of = [
        lax.ppermute(tokens, "tp", [(t, (t + step) % 4) for t in range(4)]) for step in (2, 1, 3)
    ]
    staged = (tokens, norm_gain[None], w_key, w_value, key_gain)
    staged = plain_kernel(
        stage_kernel, "stage", staged, tuple(pltpu.VMEM(a.shape, a.dtype) for a in staged), smem=0
    )
    normed_shape = jax.ShapeDtypeStruct((tok_dev, tokens.shape[1]), jnp.bfloat16)
    rows_block, own = plain_kernel(
        front_kernel,
        "front",
        (
            where,
            *staged,
            rows_of[1],
            rows_of[2],
            rows_of[0],
        ),
        (normed_shape, jax.ShapeDtypeStruct((512, 128), jnp.bfloat16)),
    )

    query_t = plain_kernel(
        query_kernel,
        "queries",
        (rows_block, w_query, query_gain.reshape(-1, 1)),
        jax.ShapeDtypeStruct((w_query.shape[1], tok_dev), jnp.bfloat16),
        smem=0,
    )
    swap = lambda z, x, c: (z, x, 1 - c)
    query_t = query_t.reshape(heads, 2 * head_dim, tok_dev)
    given = jnp.stack([query_t[3], query_t[2]])
    guest = lax.ppermute(given, "sp", mirrored((7, 6, 5)))
    partner_q = sp_send(query_t, swap)
    left = sp_send(own, lambda z, x, c: (z, x + 1, c))
    right = sp_send(own, lambda z, x, c: (z, x - 1, c))
    far = sp_send(own, lambda z, x, c: (z, x + 2, c))
    glu_a = jnp.dot(rows_block, w_glu_a, preferred_element_type=jnp.float32)
    glu_b = jnp.dot(rows_block, w_glu_b, preferred_element_type=jnp.float32)
    gated_rows = (glu_a * jax.nn.sigmoid(glu_b)).astype(jnp.bfloat16)
    prev_rows = shifted(gated_rows[tok_dev - (KW - 1) :], "sp", 1)
    guest_early, gated_rows = lax.optimization_barrier((guest, gated_rows))
    partner_guest = sp_send(guest_early, swap)
    mine = jnp.concatenate([query_t, guest_early], axis=0).reshape(-1, head_dim, tok_dev)
    other = jnp.concatenate([partner_q, partner_guest], axis=0).reshape(-1, head_dim, tok_dev)
    both_q = jnp.stack([mine, other], axis=1).reshape(-1, head_dim, tok_dev)
    slab = jnp.concatenate([own, left, right, far], axis=0)

    slab, gated_rows = lax.optimization_barrier((slab, gated_rows))
    up = sp_send(slab, lambda z, x, c: (z + 1, x, c))
    down = sp_send(slab, lambda z, x, c: (z - 1, x, c))

    padded = jnp.concatenate([prev_rows, gated_rows], axis=0)
    conv_sum = jnp.zeros((tok_dev, conv_local), jnp.float32)
    for tap_idx in range(KW):
        conv_sum = conv_sum + conv_taps[tap_idx] * padded[tap_idx : tap_idx + tok_dev].astype(
            jnp.float32
        )
    chan_total = conv_local * tp_count
    sums = jnp.concatenate([jnp.sum(conv_sum, axis=1), jnp.sum(conv_sum * conv_sum, axis=1)])
    where_0, sums = lax.optimization_barrier((where, sums))
    sums = jnp.sum(sent_to_all(sums, "tp").reshape(tp_count, -1), axis=0)
    mean_val = (sums[:tok_dev] / chan_total)[:, None]
    mean_sq = (sums[tok_dev:] / chan_total)[:, None]
    conv_out = jax.nn.silu(
        (conv_sum - mean_val) * lax.rsqrt(mean_sq - mean_val * mean_val + 1e-05) * ln_gain
    ).astype(jnp.bfloat16)
    out_part = jnp.dot(conv_out, w_out_conv, preferred_element_type=jnp.float32)

    where_2, out_part = lax.optimization_barrier((where, out_part))

    *state, spread_q = attend(where, both_q, (own, left, right, far), None, 0)
    for step in range(1, 5):
        held = sums if step == 1 else behind
        up, down, held = lax.optimization_barrier((up, down, held))
        if step > 1:
            state = (held, *state[1:])
        if step < 4:
            new_up = sp_send(up if step < 3 else up[:1024], lambda z, x, c: (z + 1, x, c))
            new_down = sp_send(down if step < 3 else down[1024:], lambda z, x, c: (z - 1, x, c))
        behind = state[0]
        if step > 1:
            state = attend(where_2 if step == 3 else where, spread_q, pending, state, step - 1)
            behind = state[0]
        pending = (up, down)
        if step < 4:
            up, down = new_up, new_down
    state = attend(where_2, spread_q, pending, state, 4)

    other_stats, other_acc = sp_send(state[1], swap), sp_send(state[3], swap)
    pairs = state[0].shape[0]
    head_out, logs = plain_kernel(
        finish_kernel,
        "finish",
        (lam_head, sub_gain[:, None], state[0], state[2], other_stats, other_acc),
        (
            jax.ShapeDtypeStruct((pairs // 2, 128, tok_dev), jnp.bfloat16),
            jax.ShapeDtypeStruct((pairs, 8, tok_dev), jnp.float32),
        ),
    )
    logs = logs[:, 0].reshape(-1, 2, tok_dev)
    back_out = lax.ppermute(head_out[heads:], "sp", mirrored((0, 1, 2)))
    back_logs = lax.ppermute(logs[heads:], "sp", mirrored((0, 1, 2)))
    z = where[0]

    def with_guests(mine, back):
        third = jnp.where(z == 7, back[1], mine[2])
        fourth = jnp.where(z >= 5, back[0], mine[3])
        return jnp.concatenate([mine[:2], third[None], fourth[None]], axis=0)

    attn_t = with_guests(head_out, back_out).reshape(heads * 128, tok_dev)
    log_sums = with_guests(logs, back_logs).transpose(1, 0, 2)

    out_part = out_part + lax.dot_general(
        attn_t, w_out_attn, (((0,), (0,)), ((), ())), preferred_element_type=jnp.float32
    )
    out_part = lax.optimization_barrier(out_part.astype(jnp.bfloat16))
    blocks = lax.all_to_all(out_part.reshape(tp_count, -1, out_part.shape[1]), "tp", 0, 0, tiled=True)
    mixed = jnp.sum(blocks.astype(jnp.float32), axis=0).astype(jnp.bfloat16)
    return (mixed, log_sums)


def solution(mesh):
    return jax.shard_map(
        on_device,
        mesh=mesh,
        in_specs=(
            P(("sp", "tp"), None),
            P(),
            P(None, "tp"),
            P(None, "tp"),
            P(None, "tp"),
            P("tp"),
            P(None, "tp"),
            P(None, "tp"),
            P(None, "tp"),
            P("tp", None),
            P("tp", None),
            P("tp"),
            P(),
            P("tp", None),
            P("tp", None),
        ),
        out_specs=(P(("sp", "tp"), None), P(None, "tp", "sp")),
        check_vma=False,
    )
```
